32 devices in a mesh: rep: 2 (over x), fs: 8 (over z, y), tp: 2 (over core).
Axes of the slice: x: 2, y: 2, z: 4, core: 2. Of those that a mesh axis runs over, the one named last changes fastest.
Arguments:
- tokens: bfloat16 [4096, 2048], P(('rep', 'fs')), may hold values from -6 to 6
- first_gain: float32 [2048], replicated, may hold values from 0.1 to 1.9
- value_weight: float32 [2048, 1024], P('fs', 'tp'), may hold values from -0.125 to 0.125
- gate_weight: float32 [2048, 1024], P('fs', 'tp'), may hold values from -0.125 to 0.125
- value_scale: float32 [1024], P('tp'), may hold values from 0.5 to 2
- gate_scale: float32 [1024], P('tp'), may hold values from 0.5 to 2
- conv_taps: float32 [31, 1024], P(None, 'tp'), may hold values from -7 to 7
- chan_gain: float32 [1024], P('tp'), may hold values from 0.1 to 1.9
- mixout_weight: float32 [1024, 2048], P('tp', 'fs'), may hold values from -0.1875 to 0.1875
- mixout_scale: float32 [2048], P('fs'), may hold values from 0.5 to 2
- second_gain: float32 [2048], replicated, may hold values from 0.1 to 1.9
- up_weight: float32 [2048, 8192], P('fs', 'tp'), may hold values from -0.125 to 0.125
- up_scale: float32 [8192], P('tp'), may hold values from 0.5 to 2
- down_weight: float32 [8192, 2048], P('tp', 'fs'), may hold values from -0.0625 to 0.0625
- down_scale: float32 [2048], P('fs'), may hold values from 0.5 to 2
Outputs:
- layer_out: bfloat16 [4096, 2048], P(('rep', 'fs'))
The draws below stay inside these ranges and needn't reach their ends.
All inputs are finite; a program needn't handle non-finite values.
Results may differ from the reference program's by a relative error of at most 0.025.
Values may be sent and summed in bfloat16 or wider, within the bound.
A program may use at most 128 MiB of HBM per device.

```python
import math
import jax
import jax.numpy as jnp
from jax import lax

D = 2048
CHANNELS = 1024
FF = 8192
CONV_K = 31
SEQ_LEN = 128
TOKENS = 4096
N_TP = 2


def draw_conv_taps(key, part):
    first, second = jax.random.split(jax.random.fold_in(key, 11))
    channel = jnp.arange(CHANNELS).astype(jnp.float32)
    rise = jnp.exp(jnp.log(6.0) * channel / max(CHANNELS - 1, 1))
    base = jnp.clip(jax.random.normal(first, (CONV_K, CHANNELS), jnp.float32), -4.0, 4.0)
    rough = jax.random.uniform(second, (CHANNELS,), jnp.float32, 0.5, 1.5)
    return (base * CONV_K ** (-0.5) * rise * rough).astype(jnp.float32)


def levels(key, dims, cuts, low, high):
    def one(dim, blocks):
        heights = jax.random.uniform(jax.random.fold_in(jax.random.fold_in(key, 6), dim), (blocks,), jnp.float32, low / len(cuts), high / len(cuts))
        return jnp.repeat(jnp.exp(heights), dims[dim] // blocks).reshape((-1,) + (1,) * (len(dims) - dim - 1))

    level = one(*cuts[0])
    for cut in cuts[1:]:
        level = level * one(*cut)
    return level


def scatter_about(own_key, extent, scale, reach, cuts=(), kind=jnp.bfloat16):
    factor_of = levels(own_key, extent, cuts, -0.22, 0.18) if cuts else 1.0
    values = jax.random.normal(own_key, extent, jnp.float32) * scale * factor_of
    return jnp.minimum(jnp.maximum(values, -reach), reach).astype(kind)


def setup_inputs(seed: int = 0) -> dict:
    keys = jax.random.split(jax.random.key(seed), 16)
    tokens = scatter_about(keys[0], (TOKENS, D), 1.0, 6.0, ((0, 16),))
    first_gain = jnp.clip(1.0 + 0.18 * jax.random.normal(keys[1], (D,), jnp.float32), 0.1, 1.9)
    value_weight = scatter_about(keys[2], (D, CHANNELS), D ** -0.5, 0.125, ((0, 8), (1, 2)), jnp.float32)
    gate_weight = scatter_about(keys[3], (D, CHANNELS), D ** -0.5, 0.125, ((0, 8), (1, 2)), jnp.float32)
    value_scale = jnp.clip(jnp.exp(math.log(2.0) - 1.3862944 * jax.random.uniform(keys[4], (CHANNELS,), jnp.float32) ** levels(keys[4], (CHANNELS,), ((0, 2),), -0.2, 0.2)), 0.5, 2.0)
    gate_scale = jnp.clip(jnp.exp(math.log(2.0) - 1.3862944 * jax.random.uniform(keys[5], (CHANNELS,), jnp.float32) ** levels(keys[5], (CHANNELS,), ((0, 2),), -0.2, 0.2)), 0.5, 2.0)
    conv_taps = draw_conv_taps(jax.random.fold_in(keys[15], 71), 0)
    chan_gain = jnp.clip(1.0 + 0.18 * jax.random.normal(keys[7], (CHANNELS,), jnp.float32), 0.1, 1.9)
    mixout_weight = scatter_about(keys[8], (CHANNELS, D), CHANNELS ** -0.5, 0.1875, ((0, 2), (1, 8)), jnp.float32)
    mixout_scale = jnp.clip(jnp.exp(math.log(2.0) - 1.3862944 * jax.random.uniform(keys[9], (D,), jnp.float32) ** levels(keys[9], (D,), ((0, 8),), -0.2, 0.2)), 0.5, 2.0)
    second_gain = jnp.clip(1.0 + 0.18 * jax.random.normal(keys[10], (D,), jnp.float32), 0.1, 1.9)
    up_weight = scatter_about(keys[11], (D, FF), D ** -0.5, 0.125, ((0, 8), (1, 2)), jnp.float32)
    up_scale = jnp.clip(jnp.exp(math.log(2.0) - 1.3862944 * jax.random.uniform(keys[12], (FF,), jnp.float32) ** levels(keys[12], (FF,), ((0, 2),), -0.2, 0.2)), 0.5, 2.0)
    down_weight = scatter_about(keys[13], (FF, D), FF ** -0.5, 0.0625, ((0, 2), (1, 8)), jnp.float32)
    down_scale = jnp.clip(jnp.exp(math.log(2.0) - 1.3862944 * jax.random.uniform(keys[14], (D,), jnp.float32) ** levels(keys[14], (D,), ((0, 8),), -0.2, 0.2)), 0.5, 2.0)
    return {"tokens": tokens, "first_gain": first_gain, "value_weight": value_weight, "gate_weight": gate_weight, "value_scale": value_scale, "gate_scale": gate_scale, "conv_taps": conv_taps, "chan_gain": chan_gain, "mixout_weight": mixout_weight, "mixout_scale": mixout_scale, "second_gain": second_gain, "up_weight": up_weight, "up_scale": up_scale, "down_weight": down_weight, "down_scale": down_scale}


def rms_rows(rows, gain):
    values = rows.astype(jnp.float32)
    scaled = values * lax.rsqrt(lax.optimization_barrier(jnp.mean(values * values, axis=-1, keepdims=True)) + 1e-05)
    return (scaled * gain).astype(jnp.bfloat16)

def rounded(scale):
    return lax.optimization_barrier(scale.astype(jnp.bfloat16)).astype(jnp.float32)

def causal_conv(signal, taps):
    width = signal.shape[1]
    seqs = signal.reshape(-1, SEQ_LEN, width)
    result = lax.conv_general_dilated(seqs, taps[:, None, :], (1,), [(taps.shape[0] - 1, 0)], dimension_numbers=('NWC', 'WIO', 'NWC'), feature_group_count=width, precision=lax.Precision.HIGHEST)
    return result.reshape(signal.shape)

def block_sum(left, right, scale):
    inner = left.shape[1] // N_TP
    total = jnp.zeros((left.shape[0], right.shape[1]), jnp.float32)
    for block in range(N_TP):
        term = jnp.dot(left[:, block * inner:(block + 1) * inner], right[block * inner:(block + 1) * inner], preferred_element_type=jnp.float32) * scale
        total = total + lax.optimization_barrier(term.astype(jnp.bfloat16)).astype(jnp.float32)
    return total

def reference(tokens, first_gain, value_weight, gate_weight, value_scale, gate_scale, conv_taps, chan_gain, mixout_weight, mixout_scale, second_gain, up_weight, up_scale, down_weight, down_scale):
    normed = rms_rows(tokens, first_gain)
    value_sum = jnp.dot(normed, value_weight.astype(jnp.bfloat16), preferred_element_type=jnp.float32)
    gate_sum = jnp.dot(normed, gate_weight.astype(jnp.bfloat16), preferred_element_type=jnp.float32)
    glu = value_sum * rounded(value_scale) * jax.nn.sigmoid(gate_sum * rounded(gate_scale))
    conv = causal_conv(glu, conv_taps)
    mean = lax.optimization_barrier(jnp.mean(conv, axis=1, keepdims=True))
    centred = conv - mean
    var = lax.optimization_barrier(jnp.mean(centred * centred, axis=1, keepdims=True))
    mixed_in = jax.nn.silu(centred * lax.rsqrt(var + 1e-05) * chan_gain).astype(jnp.bfloat16)
    mix_sum = block_sum(mixed_in, mixout_weight.astype(jnp.bfloat16), rounded(mixout_scale))
    middle = (tokens.astype(jnp.float32) + mix_sum).astype(jnp.bfloat16)
    normed2 = rms_rows(middle, second_gain)
    up_sum = jnp.dot(normed2, up_weight.astype(jnp.bfloat16), preferred_element_type=jnp.float32)
    hidden = jnp.square(jax.nn.relu(up_sum * rounded(up_scale))).astype(jnp.bfloat16)
    down_sum = block_sum(hidden, down_weight.astype(jnp.bfloat16), rounded(down_scale))
    return (middle.astype(jnp.float32) + down_sum).astype(jnp.bfloat16)
```

```python
import functools

import jax
import jax.numpy as jnp
import numpy as np
from jax import lax
from jax.sharding import PartitionSpec as P

SEQ_LEN = 128


def rms_rows(rows, gain):
    values = rows.astype(jnp.float32)
    scaled = values * lax.rsqrt(jnp.mean(values * values, axis=-1, keepdims=True) + 1e-05)
    return (scaled * gain).astype(jnp.bfloat16)


def causal_conv(signal, taps):
    width = signal.shape[1]
    seqs = signal.reshape(-1, SEQ_LEN, width)
    result = lax.conv_general_dilated(
        seqs,
        taps[:, None, :],
        (1,),
        [(taps.shape[0] - 1, 0)],
        dimension_numbers=("NWC", "WIO", "NWC"),
        feature_group_count=width,
        precision=lax.Precision.HIGHEST,
    )
    return result.reshape(signal.shape)


def on_device(
    tokens,
    first_gain,
    value_weight,
    gate_weight,
    value_scale,
    gate_scale,
    conv_taps,
    chan_gain,
    mixout_weight,
    mixout_scale,
    second_gain,
    up_weight,
    up_scale,
    down_weight,
    down_scale,
):
    normed = rms_rows(tokens, first_gain)
    count = normed.shape[0]
    width = value_weight.shape[1]
    columns = normed
    value_sum = jnp.dot(
        columns,
        lax.all_gather(value_weight.astype(jnp.bfloat16), "fs", axis=0, tiled=True),
        preferred_element_type=jnp.float32,
    )
    gate_sum = jnp.dot(
        columns,
        lax.all_gather(gate_weight.astype(jnp.bfloat16), "fs", axis=0, tiled=True),
        preferred_element_type=jnp.float32,
    )
    value_mult = value_scale.astype(jnp.bfloat16).astype(jnp.float32)
    gate_mult = gate_scale.astype(jnp.bfloat16).astype(jnp.float32)
    glu = value_sum * value_mult * jax.nn.sigmoid(gate_sum * gate_mult)
    conv = causal_conv(glu, conv_taps)
    total = width * lax.axis_size("tp")
    sums, squares = lax.psum((jnp.sum(conv, axis=1), jnp.sum(conv * conv, axis=1)), "tp")
    mean = sums / total
    var = squares / total - mean * mean
    centred = conv - mean[:, None]
    mixed_in = jax.nn.silu(centred * lax.rsqrt(var[:, None] + 1e-05) * chan_gain).astype(
        jnp.bfloat16
    )
    out_whole, out_mult = (
        lax.all_gather(mixout_weight.astype(jnp.bfloat16), "fs", axis=1, tiled=True),
        lax.all_gather(mixout_scale.astype(jnp.bfloat16), "fs", axis=0, tiled=True),
    )
    out_factor = out_mult.astype(jnp.float32)
    mix_term = jnp.dot(mixed_in, out_whole, preferred_element_type=jnp.float32) * out_factor
    mix_sum = lax.psum(mix_term.astype(jnp.bfloat16), "tp").astype(jnp.float32)
    middle = (tokens.astype(jnp.float32) + mix_sum).astype(jnp.bfloat16)
    normed2 = rms_rows(middle, second_gain)
    up_empty = jnp.zeros((count, up_weight.shape[1]), jnp.float32)
    piece = lax.all_gather(up_weight.astype(jnp.bfloat16), "fs", axis=0, tiled=True)
    columns = lax.slice_in_dim(normed2, 0, piece.shape[0], axis=1)
    up_sum = up_empty + jnp.dot(columns, piece, preferred_element_type=jnp.float32)
    up_mult = up_scale.astype(jnp.bfloat16).astype(jnp.float32)
    hidden = jnp.square(jax.nn.relu(up_sum * up_mult)).astype(jnp.bfloat16)
    down_whole, down_mult = (
        lax.all_gather(down_weight.astype(jnp.bfloat16), "fs", axis=1, tiled=True),
        lax.all_gather(down_scale.astype(jnp.bfloat16), "fs", axis=0, tiled=True),
    )
    down_factor = down_mult.astype(jnp.float32)
    down_term = jnp.dot(hidden, down_whole, preferred_element_type=jnp.float32) * down_factor
    down_sum = lax.psum(down_term.astype(jnp.bfloat16), "tp").astype(jnp.float32)
    return (middle.astype(jnp.float32) + down_sum).astype(jnp.bfloat16)


def ring_order(mesh):
    axis = mesh.axis_names.index("fs")
    line = np.moveaxis(mesh.devices, axis, 0).reshape(mesh.shape["fs"], -1)[:, 0]
    places = [getattr(d, "coords", None) for d in line]
    if any(p is None for p in places):
        return list(range(len(places)))
    at = {(p[2], p[1]): i for i, p in enumerate(places)}
    zs, ys = sorted({k[0] for k in at}), sorted({k[1] for k in at})
    if len(at) != len(zs) * len(ys) or len(zs) % 2 or len(ys) < 2:
        return list(range(len(places)))
    order = []
    for row, z in enumerate(zs):
        order += [at[z, y] for y in (ys[1:] if row % 2 == 0 else ys[:0:-1])]
    return order + [at[z, ys[0]] for z in reversed(zs)]


def pick(table, index):
    return jnp.asarray(table, jnp.int32)[index]


def ring_device(order, *args):
    (
        tokens,
        first_gain,
        value_weight,
        gate_weight,
        value_scale,
        gate_scale,
        conv_taps,
        chan_gain,
        mixout_weight,
        mixout_scale,
        second_gain,
        up_weight,
        up_scale,
        down_weight,
        down_scale,
    ) = args
    f32, b16 = jnp.float32, jnp.bfloat16
    n = lax.axis_size("fs")
    half_way = n // 2
    here = lax.axis_index("fs")
    first_rep = lax.axis_index("rep") == 0
    first_tp = lax.axis_index("tp") == 0
    place_of = [order.index(i) for i in range(n)]
    place = pick(place_of, here)

    def owner(offset):
        return pick(order, (place + offset) % n)

    def shift(block, step):
        return lax.ppermute(
            block, "fs", [(order[p], order[(p + step) % n]) for p in range(n)]
        )

    def across(block, axis):
        return lax.ppermute(block, axis, [(0, 1), (1, 0)])

    def ring_gather(block, axis=0):
        size = block.shape[axis] // 2
        got = {0: block}
        low = high = block
        for step in range(1, half_way):
            low, high = shift(low, 1), shift(high, -1)
            got[n - step], got[step] = low, high
        one = lax.slice_in_dim(low, 0, size, axis=axis)
        two = lax.slice_in_dim(high, size, 2 * size, axis=axis)
        got[half_way] = jnp.concatenate([shift(one, 1), shift(two, -1)], axis=axis)
        return [got[k] for k in range(n)]

    def ring_scatter(part):
        far = part(half_way)
        size = far.shape[1] // 2
        low, high = shift(far[:, :size].astype(b16), 1), shift(far[:, size:].astype(b16), -1)
        for step in range(half_way - 1, 0, -1):
            up, down = part(step), part(n - step)
            if step == half_way - 1:
                up = up + jnp.pad(low.astype(f32), ((0, 0), (0, size)))
                down = down + jnp.pad(high.astype(f32), ((0, 0), (size, 0)))
            else:
                up, down = up + low.astype(f32), down + high.astype(f32)
            low, high = shift(up.astype(b16), 1), shift(down.astype(b16), -1)
        return part(0) + low.astype(f32) + high.astype(f32)

    mine = jnp.where(first_rep, value_weight, gate_weight).astype(b16)
    other = jnp.where(first_rep, gate_weight, value_weight).astype(b16)
    mine_all = ring_gather(mine)
    other_all = [other] + [across(block, "rep") for block in mine_all[1:]]
    out_piece = (mixout_weight.astype(b16).astype(f32) * mixout_scale.astype(b16).astype(f32)).astype(b16)

    depth, wide = up_weight.shape[0], up_weight.shape[1] // n
    up_cut = up_weight.reshape(depth, n, wide).transpose(1, 0, 2)
    down_scaled = down_weight.astype(b16).astype(f32) * down_scale.astype(b16).astype(f32)
    down_cut = down_scaled.reshape(n, wide, down_weight.shape[1])
    down_cut = jnp.concatenate([down_cut[:, : wide // 2], down_cut[:, wide // 2 :]], axis=2)
    own_cut = jnp.where(first_rep, up_cut, down_cut).astype(b16)
    rest_cut = jnp.where(first_rep, down_cut, up_cut).astype(b16)
    out_pieces = ring_gather(out_piece, axis=1)

    normed = rms_rows(tokens, first_gain)
    width = value_weight.shape[1]
    normed_turned = jnp.concatenate(
        [lax.dynamic_slice_in_dim(normed, owner(k) * depth, depth, axis=1) for k in range(n)], axis=1
    )
    mine_sum = jnp.dot(
        normed_turned, jnp.concatenate(mine_all, axis=0), preferred_element_type=f32
    )
    other_sum = jnp.dot(
        normed_turned, jnp.concatenate(other_all, axis=0), preferred_element_type=f32
    )

    sent = []
    for k in range(1, n):
        block = lax.dynamic_index_in_dim(own_cut, owner(k), 0, keepdims=False)
        sent.append(shift(block, k))
    own_pieces = [lax.dynamic_index_in_dim(own_cut, here, 0, keepdims=False)] + sent[::-1]
    rest_pieces = [lax.dynamic_index_in_dim(rest_cut, here, 0, keepdims=False)] + [
        across(block, "rep") for block in own_pieces[1:]
    ]
    own_stack, rest_stack = jnp.stack(own_pieces), jnp.stack(rest_pieces)

    value_sum = jnp.where(first_rep, mine_sum, other_sum)
    gate_sum = jnp.where(first_rep, other_sum, mine_sum)
    value_mult = value_scale.astype(b16).astype(f32)
    gate_mult = gate_scale.astype(b16).astype(f32)
    glu = value_sum * value_mult * jax.nn.sigmoid(gate_sum * gate_mult)
    conv = causal_conv(glu, conv_taps)
    total = width * lax.axis_size("tp")
    stats = jnp.stack([jnp.sum(conv, axis=1), jnp.sum(conv * conv, axis=1)])
    sums, squares = stats + across(stats, "tp")
    mean = sums / total
    var = squares / total - mean * mean
    centred = conv - mean[:, None]
    mixed_in = jax.nn.silu(centred * lax.rsqrt(var[:, None] + 1e-05) * chan_gain).astype(b16)
    mix_turned = jnp.dot(
        mixed_in, jnp.concatenate(out_pieces, axis=1), preferred_element_type=f32
    ).astype(b16)
    cols = out_piece.shape[1]
    mix_term = jnp.concatenate(
        [
            lax.dynamic_slice_in_dim(mix_turned, (place_of[j] - place) % n * cols, cols, axis=1)
            for j in range(n)
        ],
        axis=1,
    )
    mix_sum = mix_term.astype(f32) + across(mix_term, "tp").astype(f32)
    middle = (tokens.astype(f32) + mix_sum).astype(b16)
    normed2 = rms_rows(middle, second_gain)

    count = normed2.shape[0] // 2
    sel = lax.axis_index("tp") * count
    own_rows = lax.dynamic_slice_in_dim(normed2, sel, count, axis=0)
    their_rows = lax.dynamic_slice_in_dim(normed2, count - sel, count, axis=0)
    ours = ring_gather(own_rows, axis=1)
    theirs = [their_rows] + [across(block, "tp") for block in ours[1:]]

    def straight(stack):
        return [
            lax.dynamic_index_in_dim(stack, (place_of[j] - place) % n, 0, keepdims=False)
            for j in range(n)
        ]

    own_flat = jnp.stack(straight(own_stack))
    rest_flat = jnp.stack(straight(rest_stack))
    up_flat = jnp.where(first_rep, own_flat, rest_flat).reshape(n * depth, wide)
    down_flat = jnp.where(first_rep, rest_flat, own_flat)
    down_flat = down_flat.reshape(n, wide // 2, 2, cols).transpose(2, 1, 0, 3).reshape(wide, n * cols)
    mult = lax.dynamic_slice_in_dim(up_scale.astype(b16).astype(f32), here * wide, wide)

    def feed(rows):
        hidden = jnp.square(jax.nn.relu(jnp.dot(rows, up_flat, preferred_element_type=f32) * mult))
        return jnp.dot(hidden.astype(b16), down_flat, preferred_element_type=f32)

    their_terms = feed(jnp.concatenate(theirs, axis=0)).astype(b16)
    our_terms = feed(jnp.concatenate(ours, axis=0)).astype(b16)
    passed = across(their_terms, "tp")

    def part(k):
        rows = slice(k * count, (k + 1) * count)
        return our_terms[rows].astype(f32) + passed[rows].astype(f32)

    down_rows = ring_scatter(part)
    ours_out = lax.dynamic_slice_in_dim(middle, sel, count, axis=0).astype(f32) + down_rows
    ours_out = ours_out.astype(b16)
    theirs_out = across(ours_out, "tp")
    return jnp.where(
        first_tp,
        jnp.concatenate([ours_out, theirs_out], axis=0),
        jnp.concatenate([theirs_out, ours_out], axis=0),
    )


def solution(mesh):
    placed = (
        P(("rep", "fs"), None),
        P(),
        P("fs", "tp"),
        P("fs", "tp"),
        P("tp"),
        P("tp"),
        P(None, "tp"),
        P("tp"),
        P("tp", "fs"),
        P("fs"),
        P(),
        P("fs", "tp"),
        P("tp"),
        P("tp", "fs"),
        P("fs"),
    )
    n = mesh.shape["fs"]
    small = mesh.shape["rep"] == 2 and mesh.shape["tp"] == 2 and n % 2 == 0 and 4 <= n <= 16
    body = functools.partial(ring_device, ring_order(mesh)) if small else on_device
    return jax.shard_map(
        body, mesh=mesh, in_specs=placed, out_specs=P(("rep", "fs"), None), check_vma=False
    )
```

```python
import functools

import jax
import jax.numpy as jnp
import numpy as np
from jax import lax
from jax.experimental import pallas as pl
from jax.experimental.pallas import tpu as pltpu
from jax.sharding import PartitionSpec as P

SEQ_LEN = 128


def rms_rows(rows, gain):
    values = rows.astype(jnp.float32)
    scaled = values * lax.rsqrt(jnp.mean(values * values, axis=-1, keepdims=True) + 1e-05)
    return (scaled * gain).astype(jnp.bfloat16)


def causal_conv(signal, taps):
    width = signal.shape[1]
    seqs = signal.reshape(-1, SEQ_LEN, width)
    result = lax.conv_general_dilated(
        seqs,
        taps[:, None, :],
        (1,),
        [(taps.shape[0] - 1, 0)],
        dimension_numbers=("NWC", "WIO", "NWC"),
        feature_group_count=width,
        precision=lax.Precision.HIGHEST,
    )
    return result.reshape(signal.shape)


def on_device(
    tokens,
    first_gain,
    value_weight,
    gate_weight,
    value_scale,
    gate_scale,
    conv_taps,
    chan_gain,
    mixout_weight,
    mixout_scale,
    second_gain,
    up_weight,
    up_scale,
    down_weight,
    down_scale,
):
    normed = rms_rows(tokens, first_gain)
    count = normed.shape[0]
    width = value_weight.shape[1]
    columns = normed
    value_sum = jnp.dot(
        columns,
        lax.all_gather(value_weight.astype(jnp.bfloat16), "fs", axis=0, tiled=True),
        preferred_element_type=jnp.float32,
    )
    gate_sum = jnp.dot(
        columns,
        lax.all_gather(gate_weight.astype(jnp.bfloat16), "fs", axis=0, tiled=True),
        preferred_element_type=jnp.float32,
    )
    value_mult = value_scale.astype(jnp.bfloat16).astype(jnp.float32)
    gate_mult = gate_scale.astype(jnp.bfloat16).astype(jnp.float32)
    glu = value_sum * value_mult * jax.nn.sigmoid(gate_sum * gate_mult)
    conv = causal_conv(glu, conv_taps)
    total = width * lax.axis_size("tp")
    sums, squares = lax.psum((jnp.sum(conv, axis=1), jnp.sum(conv * conv, axis=1)), "tp")
    mean = sums / total
    var = squares / total - mean * mean
    centred = conv - mean[:, None]
    mixed_in = jax.nn.silu(centred * lax.rsqrt(var[:, None] + 1e-05) * chan_gain).astype(
        jnp.bfloat16
    )
    out_whole, out_mult = (
        lax.all_gather(mixout_weight.astype(jnp.bfloat16), "fs", axis=1, tiled=True),
        lax.all_gather(mixout_scale.astype(jnp.bfloat16), "fs", axis=0, tiled=True),
    )
    out_factor = out_mult.astype(jnp.float32)
    mix_term = jnp.dot(mixed_in, out_whole, preferred_element_type=jnp.float32) * out_factor
    mix_sum = lax.psum(mix_term.astype(jnp.bfloat16), "tp").astype(jnp.float32)
    middle = (tokens.astype(jnp.float32) + mix_sum).astype(jnp.bfloat16)
    normed2 = rms_rows(middle, second_gain)
    up_empty = jnp.zeros((count, up_weight.shape[1]), jnp.float32)
    piece = lax.all_gather(up_weight.astype(jnp.bfloat16), "fs", axis=0, tiled=True)
    columns = lax.slice_in_dim(normed2, 0, piece.shape[0], axis=1)
    up_sum = up_empty + jnp.dot(columns, piece, preferred_element_type=jnp.float32)
    up_mult = up_scale.astype(jnp.bfloat16).astype(jnp.float32)
    hidden = jnp.square(jax.nn.relu(up_sum * up_mult)).astype(jnp.bfloat16)
    down_whole, down_mult = (
        lax.all_gather(down_weight.astype(jnp.bfloat16), "fs", axis=1, tiled=True),
        lax.all_gather(down_scale.astype(jnp.bfloat16), "fs", axis=0, tiled=True),
    )
    down_factor = down_mult.astype(jnp.float32)
    down_term = jnp.dot(hidden, down_whole, preferred_element_type=jnp.float32) * down_factor
    down_sum = lax.psum(down_term.astype(jnp.bfloat16), "tp").astype(jnp.float32)
    return (middle.astype(jnp.float32) + down_sum).astype(jnp.bfloat16)


def ring_order(mesh):
    axis = mesh.axis_names.index("fs")
    line = np.moveaxis(mesh.devices, axis, 0).reshape(mesh.shape["fs"], -1)[:, 0]
    places = [getattr(d, "coords", None) for d in line]
    if any(p is None for p in places):
        return list(range(len(places)))
    at = {(p[2], p[1]): i for i, p in enumerate(places)}
    zs, ys = sorted({k[0] for k in at}), sorted({k[1] for k in at})
    if len(at) != len(zs) * len(ys) or len(zs) % 2 or len(ys) < 2:
        return list(range(len(places)))
    order = []
    for row, z in enumerate(zs):
        order += [at[z, y] for y in (ys[1:] if row % 2 == 0 else ys[:0:-1])]
    return order + [at[z, ys[0]] for z in reversed(zs)]


MESH = pl.DeviceIdType.MESH
F32, B16 = jnp.float32, jnp.bfloat16


def pick(table, index):
    value = jnp.int32(table[0])
    for i in range(1, len(table)):
        value = jnp.where(index == i, jnp.int32(table[i]), value)
    return value


def remote(src, dst, send_sem, recv_sem, target):
    return pltpu.make_async_remote_copy(
        src_ref=src,
        dst_ref=dst,
        send_sem=send_sem,
        recv_sem=recv_sem,
        device_id=target,
        device_id_type=MESH,
    )


def greet(targets):
    barrier = pltpu.get_barrier_semaphore()
    for target in targets:
        pl.semaphore_signal(barrier, inc=1, device_id=target, device_id_type=MESH)
    pl.semaphore_wait(barrier, len(targets))


def ring_targets(order):
    n = len(order)
    here = lax.axis_index("fs")
    up = pick([order[(order.index(i) + 1) % n] for i in range(n)], here)
    down = pick([order[(order.index(i) - 1) % n] for i in range(n)], here)
    return {"fs": up}, {"fs": down}


def ring_round(n, block, half, sems, up, down, landed=None):
    send, recv = sems
    middle = n // 2
    started = []
    for step in range(1, middle + 1):
        pair = []
        if step < middle:
            low_from, high_from = block((n - step + 1) % n), block(step - 1)
            low_to, high_to = block(n - step), block(step)
        else:
            low_from, high_from = half((n - step + 1) % n, 0), half(step - 1, 1)
            low_to, high_to = half(middle, 0), half(middle, 1)
        low_sem, high_sem = n - step, (step if step < middle else n)
        pair.append(remote(low_from, low_to, send.at[low_sem], recv.at[low_sem], up))
        pair.append(remote(high_from, high_to, send.at[high_sem], recv.at[high_sem], down))
        for copy in pair:
            copy.start()
        started += pair
        yield
        for copy in pair:
            copy.wait_recv()
        if landed is not None:
            for k in [n - step, step] if step < middle else [middle]:
                landed(k)
    for copy in started:
        copy.wait_send()


def run_together(rounds):
    live = list(rounds)
    while live:
        for one in list(live):
            try:
                next(one)
            except StopIteration:
                live.remove(one)


def weights_kernel(order, mine, other, piece, cut, rest, mine_all, other_all, piece_all, own_flat, rest_flat,
                   ring_send, ring_recv, out_send, out_recv, x_send, x_recv, cut_send, cut_recv, swap_send, swap_recv, local):
    n = len(order)
    here, rep = lax.axis_index("fs"), lax.axis_index("rep")
    up, down = ring_targets(order)
    partner = {"rep": 1 - rep}
    peers = [{"fs": lax.rem(here + k, n)} for k in range(1, n)]
    greet(peers + [partner])
    rows, cols = mine.shape[0], piece.shape[1]

    def first(k):
        return mine if k == 0 else mine_all.at[pl.ds(k * rows, rows)]

    def first_half(k, i):
        size = rows // 2
        if k == 0:
            return mine.at[pl.ds(i * size, size)]
        return mine_all.at[pl.ds(k * rows + i * size, size)]

    def second(k):
        return piece if k == 0 else piece_all.at[:, pl.ds(k * cols, cols)]

    def second_half(k, i):
        size = piece.shape[0] // 2
        if k == 0:
            return piece.at[pl.ds(i * size, size)]
        return piece_all.at[pl.ds(i * size, size), pl.ds(k * cols, cols)]

    crossing = []

    def landed(k):
        there = pl.ds(k * rows, rows)
        copy = remote(mine_all.at[there], other_all.at[there], x_send.at[k], x_recv.at[k], partner)
        copy.start()
        crossing.append(copy)

    kept = [
        pltpu.make_async_copy(mine, mine_all.at[pl.ds(0, rows)], local.at[0]),
        pltpu.make_async_copy(other, other_all.at[pl.ds(0, rows)], local.at[1]),
        pltpu.make_async_copy(piece, piece_all.at[:, pl.ds(0, cols)], local.at[2]),
        pltpu.make_async_copy(cut.at[here], own_flat.at[here], local.at[3]),
        pltpu.make_async_copy(rest, rest_flat.at[here], local.at[4]),
    ]
    for copy in kept:
        copy.start()
    run_together(
        [
            ring_round(n, first, first_half, (ring_send, ring_recv), up, down, landed),
            ring_round(n, second, second_half, (out_send, out_recv), up, down),
        ]
    )
    sends = []
    for k in range(1, n):
        to = lax.rem(here + k, n)
        copy = remote(cut.at[to], own_flat.at[here], cut_send.at[k], cut_recv.at[k], {"fs": to})
        copy.start()
        sends.append(copy)
    swaps = []
    for k in range(1, n):
        sends[k - 1].wait_recv()
        came = lax.rem(here - k + n, n)
        copy = remote(own_flat.at[came], rest_flat.at[came], swap_send.at[k], swap_recv.at[k], partner)
        copy.start()
        swaps.append(copy)
    for copy in sends:
        copy.wait_send()
    for copy in crossing + swaps:
        copy.wait()
    for copy in kept:
        copy.wait()


def tokens_kernel(order, rows_ref, ours, theirs, ring_send, ring_recv, tp_send, tp_recv, local):
    n = len(order)
    tp = lax.axis_index("tp")
    up, down = ring_targets(order)
    partner = {"tp": 1 - tp}
    greet([up, down, partner])
    count, wide = rows_ref.shape[0] // 2, rows_ref.shape[1]
    own = pl.ds(pl.multiple_of(tp * count, count), count)
    rest = pl.ds(pl.multiple_of((1 - tp) * count, count), count)

    def block(k):
        return rows_ref.at[own] if k == 0 else ours.at[pl.ds(k * count, count)]

    def half(k, i):
        size = wide // 2
        if k == 0:
            return rows_ref.at[own, pl.ds(i * size, size)]
        return ours.at[pl.ds(k * count, count), pl.ds(i * size, size)]

    crossing = []

    def landed(k):
        there = pl.ds(k * count, count)
        copy = remote(ours.at[there], theirs.at[there], tp_send.at[k], tp_recv.at[k], partner)
        copy.start()
        crossing.append(copy)

    kept = [
        pltpu.make_async_copy(rows_ref.at[own], ours.at[pl.ds(0, count)], local.at[0]),
        pltpu.make_async_copy(rows_ref.at[rest], theirs.at[pl.ds(0, count)], local.at[1]),
    ]
    for copy in kept:
        copy.start()
    run_together([ring_round(n, block, half, (ring_send, ring_recv), up, down, landed)])
    for copy in crossing + kept:
        copy.wait()


def sums_kernel(order, ours, theirs, middle, out, passed, going, coming, tp_send, tp_recv,
                ring_send, ring_recv, last):
    n = len(order)
    half_way = n // 2
    tp = lax.axis_index("tp")
    up, down = ring_targets(order)
    partner = {"tp": 1 - tp}
    greet([up, down, partner])
    count, wide = middle.shape[0] // 2, middle.shape[1]
    size = wide // 2
    needed = [half_way]
    for step in range(half_way - 1, 0, -1):
        needed += [step, n - step]
    needed.append(0)
    passing = {}
    for k in needed:
        there = pl.ds(k * count, count)
        passing[k] = remote(theirs.at[there], passed.at[there], tp_send.at[k], tp_recv.at[k], partner)
        passing[k].start()

    def part(k, cols=slice(None)):
        there = slice(k * count, (k + 1) * count)
        return ours[there, cols].astype(F32) + passed[there, cols].astype(F32)

    halves = (pl.ds(0, size), pl.ds(size, size))
    flights = []
    passing[half_way].wait_recv()
    far = part(half_way)
    for way, target in enumerate((up, down)):
        going[way, 0, :, way * size : (way + 1) * size] = far[:, way * size : (way + 1) * size].astype(B16)
        copy = remote(
            going.at[way, 0, :, halves[way]],
            coming.at[way, 0, :, halves[way]],
            ring_send.at[way, 0],
            ring_recv.at[way, 0],
            target,
        )
        copy.start()
        flights.append(copy)
    pair = flights[-2:]
    for hop, step in enumerate(range(half_way - 1, 0, -1), 1):
        fresh = []
        for way, target in enumerate((up, down)):
            k = step if way == 0 else n - step
            passing[k].wait_recv()
            pair[way].wait_recv()
            if hop == 1:
                near = slice(way * size, (way + 1) * size)
                other = slice((1 - way) * size, (2 - way) * size)
                going[way, hop, :, near] = (part(k, near) + coming[way, 0, :, near].astype(F32)).astype(B16)
                going[way, hop, :, other] = part(k, other).astype(B16)
            else:
                going[way, hop] = (part(k) + coming[way, hop - 1].astype(F32)).astype(B16)
            copy = remote(
                going.at[way, hop], coming.at[way, hop], ring_send.at[way, hop], ring_recv.at[way, hop], target
            )
            copy.start()
            fresh.append(copy)
        flights += fresh
        pair = fresh
    passing[0].wait_recv()
    for copy in pair:
        copy.wait_recv()
    hop = half_way - 1
    total = part(0) + coming[0, hop].astype(F32) + coming[1, hop].astype(F32)
    own = pl.ds(pl.multiple_of(tp * count, count), count)
    out[own, :] = (middle[own, :].astype(F32) + total).astype(B16)
    final = remote(out.at[own], out.at[own], last.at[0], last.at[1], partner)
    final.start()
    for copy in passing.values():
        copy.wait_send()
    for copy in flights:
        copy.wait_send()
    final.wait()


def call(kernel, outs, scratch, number, *operands):
    spec = pl.BlockSpec(memory_space=pltpu.VMEM)
    return pl.pallas_call(
        kernel,
        out_shape=[jax.ShapeDtypeStruct(shape, B16) for shape in outs],
        in_specs=[spec] * len(operands),
        out_specs=[spec] * len(outs),
        scratch_shapes=scratch,
        compiler_params=pltpu.CompilerParams(
            collective_id=number, has_side_effects=True, vmem_limit_bytes=56 * 1024 * 1024
        ),
    )(*operands)


def ring_device(order, *args):
    (
        tokens,
        first_gain,
        value_weight,
        gate_weight,
        value_scale,
        gate_scale,
        conv_taps,
        chan_gain,
        mixout_weight,
        mixout_scale,
        second_gain,
        up_weight,
        up_scale,
        down_weight,
        down_scale,
    ) = args
    f32, b16 = jnp.float32, jnp.bfloat16
    n = lax.axis_size("fs")
    here = lax.axis_index("fs")
    first_rep = lax.axis_index("rep") == 0
    place_of = [order.index(i) for i in range(n)]
    place = pick(place_of, here)

    def owner(offset):
        return pick(order, (place + offset) % n)

    def across(block, axis):
        return lax.ppermute(block, axis, [(0, 1), (1, 0)])

    mine = jnp.where(first_rep, value_weight, gate_weight).astype(b16)
    other = jnp.where(first_rep, gate_weight, value_weight).astype(b16)
    out_piece = (mixout_weight.astype(b16).astype(f32) * mixout_scale.astype(b16).astype(f32)).astype(b16)

    depth, wide = up_weight.shape[0], up_weight.shape[1] // n
    up_cut = jnp.stack([up_weight[:, k * wide : (k + 1) * wide] for k in range(n)])
    down_scaled = down_weight.astype(b16).astype(f32) * down_scale.astype(b16).astype(f32)
    down_cut = down_scaled.reshape(n, wide, down_weight.shape[1])
    down_cut = jnp.concatenate([down_cut[:, : wide // 2], down_cut[:, wide // 2 :]], axis=2)
    own_cut = jnp.where(first_rep, up_cut, down_cut).astype(b16)
    rest_cut = jnp.where(first_rep, down_cut, up_cut).astype(b16)
    here_rest = lax.dynamic_index_in_dim(rest_cut, here, 0, keepdims=False)
    rows, cols = mine.shape[0], out_piece.shape[1]
    dma = pltpu.SemaphoreType.DMA
    mine_all, other_all, out_all, own_flat, rest_flat = call(
        functools.partial(weights_kernel, order),
        [(n * rows, mine.shape[1])] * 2 + [(out_piece.shape[0], n * cols)] + [own_cut.shape] * 2,
        [dma((n + 1,))] * 4 + [dma((n,))] * 6 + [dma((5,))],
        0,
        mine,
        other,
        out_piece,
        own_cut,
        here_rest,
    )

    normed = rms_rows(tokens, first_gain)
    width = value_weight.shape[1]
    normed_turned = jnp.concatenate(
        [lax.dynamic_slice_in_dim(normed, owner(k) * depth, depth, axis=1) for k in range(n)], axis=1
    )
    mine_sum = jnp.dot(
        normed_turned, mine_all, preferred_element_type=f32
    )
    other_sum = jnp.dot(
        normed_turned, other_all, preferred_element_type=f32
    )

    value_sum = jnp.where(first_rep, mine_sum, other_sum)
    gate_sum = jnp.where(first_rep, other_sum, mine_sum)
    value_mult = value_scale.astype(b16).astype(f32)
    gate_mult = gate_scale.astype(b16).astype(f32)
    glu = value_sum * value_mult * jax.nn.sigmoid(gate_sum * gate_mult)
    conv = causal_conv(glu, conv_taps)
    total = width * lax.axis_size("tp")
    stats = jnp.stack([jnp.sum(conv, axis=1), jnp.sum(conv * conv, axis=1)])
    sums, squares = stats + across(stats, "tp")
    mean = sums / total
    var = squares / total - mean * mean
    centred = conv - mean[:, None]
    mixed_in = jax.nn.silu(centred * lax.rsqrt(var[:, None] + 1e-05) * chan_gain).astype(b16)
    mix_turned = jnp.dot(
        mixed_in, out_all, preferred_element_type=f32
    ).astype(b16)
    mix_term = jnp.concatenate(
        [
            lax.dynamic_slice_in_dim(mix_turned, (place_of[j] - place) % n * cols, cols, axis=1)
            for j in range(n)
        ],
        axis=1,
    )
    mix_sum = mix_term.astype(f32) + across(mix_term, "tp").astype(f32)
    middle = (tokens.astype(f32) + mix_sum).astype(b16)
    normed2 = rms_rows(middle, second_gain)

    count = normed2.shape[0] // 2
    ours, theirs = call(
        functools.partial(tokens_kernel, order),
        [(n * count, normed2.shape[1])] * 2,
        [dma((n + 1,))] * 2 + [dma((n,))] * 2 + [dma((2,))],
        1,
        normed2,
    )
    up_flat = jnp.where(first_rep, own_flat, rest_flat).reshape(n * depth, wide)
    down_flat = jnp.where(first_rep, rest_flat, own_flat)
    down_flat = jnp.concatenate(
        [jnp.concatenate([block[:, :cols], block[:, cols:]], axis=0) for block in down_flat], axis=1
    )
    mult = lax.dynamic_slice_in_dim(up_scale.astype(b16).astype(f32), here * wide, wide)

    def feed(rows):
        hidden = jnp.square(jax.nn.relu(jnp.dot(rows, up_flat, preferred_element_type=f32) * mult))
        return jnp.dot(hidden.astype(b16), down_flat, preferred_element_type=f32)

    half_way = n // 2
    full = (2, half_way, count, normed2.shape[1])
    (result,) = call(
        functools.partial(sums_kernel, order),
        [middle.shape],
        [
            pltpu.VMEM((n * count, normed2.shape[1]), b16),
            pltpu.VMEM(full, b16),
            pltpu.VMEM(full, b16),
            dma((n,)),
            dma((n,)),
            dma((2, half_way)),
            dma((2, half_way)),
            dma((2,)),
        ],
        2,
        feed(ours).astype(b16),
        feed(theirs).astype(b16),
        middle,
    )
    return result


def solution(mesh):
    placed = (
        P(("rep", "fs"), None),
        P(),
        P("fs", "tp"),
        P("fs", "tp"),
        P("tp"),
        P("tp"),
        P(None, "tp"),
        P("tp"),
        P("tp", "fs"),
        P("fs"),
        P(),
        P("fs", "tp"),
        P("tp"),
        P("tp", "fs"),
        P("fs"),
    )
    n = mesh.shape["fs"]
    small = mesh.shape["rep"] == 2 and mesh.shape["tp"] == 2 and n % 2 == 0 and 4 <= n <= 16
    body = functools.partial(ring_device, ring_order(mesh)) if small else on_device
    return jax.shard_map(
        body, mesh=mesh, in_specs=placed, out_specs=P(("rep", "fs"), None), check_vma=False
    )
```
